32 devices in a mesh: ep: 8 (over z, x), tp: 4 (over y, core).
Axes of the slice: x: 2, y: 2, z: 4, core: 2. Of those that a mesh axis runs over, the one named last changes fastest.
Arguments:
- tokens: bfloat16 [64, 2048], P(('ep', 'tp')), may hold values from -6 to 6
- cache_keys: bfloat16 [64, 1024, 256], P(('ep', 'tp')), may hold values from -360 to 360
- cache_values: bfloat16 [64, 1024, 256], P(('ep', 'tp')), may hold values from -6 to 6
- cache_gates: float32 [64, 2, 1024], P(('ep', 'tp')), may hold values from -256 to 0, as said below
- lengths: int32 [64], P(('ep', 'tp')), may hold values from 1 to 1024, 32768 in all
- routes: int32 [64, 4], P(('ep', 'tp')), may hold values from 0 to 7, all different within a row; in each aligned block of 2 rows (0 to 1, 2 to 3, ...) no two rows name the same one
- route_logits: float32 [64, 4], P(('ep', 'tp')), may hold values from -6 to 6
- attn_gain: float32 [2048], replicated, may hold values from 0.1 to 1.9
- w_query: bfloat16 [2048, 2048], P(None, 'tp'), may hold values from -0.125 to 0.125
- w_keyval: bfloat16 [2048, 512], P(None, 'tp'), may hold values from -0.125 to 0.125
- w_forget: bfloat16 [2048, 2], replicated, may hold values from -0.125 to 0.125
- forget_bias: float32 [2], replicated, may hold values from -1 to 3
- w_out: bfloat16 [2048, 2048], P(None, 'tp'), may hold values from -0.125 to 0.125
- mix_gain: float32 [2048], replicated, may hold values from 0.1 to 1.9
- ffn_gain: float32 [2048], replicated, may hold values from 0.1 to 1.9
- w_gate: bfloat16 [8, 2048, 2048], P('ep', None, 'tp'), may hold values from -0.125 to 0.125
- w_lin: bfloat16 [8, 2048, 2048], P('ep', None, 'tp'), may hold values from -0.125 to 0.125
- gate_bias: float32 [8, 2048], P('ep', 'tp'), may hold values from -12 to 12
- lin_bias: float32 [8, 2048], P('ep', 'tp'), may hold values from -12 to 12
- w_down: bfloat16 [8, 2048, 2048], P('ep', 'tp'), may hold values from -0.125 to 0.125
- post_gain: float32 [2048], replicated, may hold values from 0.1 to 1.9
Outputs:
- updated: bfloat16 [64, 2048], P(('ep', 'tp'))
- new_entries: bfloat16 [64, 512], P(('ep', 'tp'))
The draws below stay inside these ranges and needn't reach their ends.
Inputs may be any that keep to these rules, and one draw needn't show every extreme that they name: `cache_gates`: along the positions of each sequence and head the values never increase. The lengths of all sequences add up to 32768, and some sequence has exactly 1024. `routes`: each row names 4 different experts; among the rows of one device no expert is named twice; every expert is named by some row.
All inputs are finite; a program needn't handle non-finite values. No bound on the sum of `lengths` on one device may be relied on, other than what follows from the above.
Results may differ from the reference program's by a relative error of at most 0.014.
The reference program's roundings to bfloat16 on the way count: a program that leaves them out, or rounds other values in their place, can miss the bound.
Values may be sent and summed in bfloat16 or wider, within the bound.
A program may use at most 64 MiB of HBM per device.

```python
import math
import jax
import jax.numpy as jnp
import numpy as np
from jax import lax

D = 2048
HEADS = 16
KVH = 2
HDIM = 128
FF = 2048
TOPK = 4
SEQ_DEV = 2
LEN = 1024
TOKENS = 64
EXPERTS = 8
N_TP = 4


def draw_cache_keys(key, part):
    first = jax.random.fold_in(jax.random.fold_in(key, 11), 0)
    values = jax.random.normal(first, (TOKENS, LEN, KVH * HDIM), jnp.float32)
    return jnp.clip(values, -360.0, 360.0).astype(jnp.bfloat16)


def draw_cache_gates(key, part):
    parts = jax.random.split(jax.random.fold_in(key, 23), 6)
    span = 32
    noise = jax.random.uniform(parts[0], (TOKENS, KVH, LEN), jnp.float32, 0.5, 1.5)
    blocks = jnp.exp(jax.random.uniform(parts[1], (TOKENS, 1, LEN // span), jnp.float32, -0.7, 0.7))
    blocks = jnp.repeat(blocks, span, axis=2)
    per_seq = jnp.exp(jax.random.uniform(parts[2], (TOKENS, 1, 1), jnp.float32, -0.7, 0.7))
    share = 0.5
    slow = jax.random.uniform(parts[3], (TOKENS, KVH, 1), jnp.float32) < share
    fast_rate = jnp.exp(jax.random.uniform(parts[4], (TOKENS, KVH, 1), jnp.float32, math.log(1.0 / 60.0), math.log(1.0 / 30.0)))
    slow_rate = jnp.exp(jax.random.uniform(parts[5], (TOKENS, KVH, 1), jnp.float32, -0.7, 0.0)) / LEN
    rate = jnp.where(slow, slow_rate, fast_rate)
    return jnp.cumsum(-rate * noise * blocks * per_seq, axis=2)


def block_levels(own_key, extent, cuts, smallest, largest):
    level, own = 1.0, jax.random.fold_in(own_key, 6)
    for axis_at, blocks in cuts:
        draws = jnp.exp(jax.random.uniform(jax.random.fold_in(own, axis_at), (blocks,), jnp.float32, smallest / len(cuts), largest / len(cuts)))
        level = level * jnp.repeat(draws, extent[axis_at] // blocks).reshape([-1 if axis == axis_at else 1 for axis in range(len(extent))])
    return level


def split_up(number_of, total, bound, lean):
    loads = [(1 << 20) // math.isqrt(grade ** lean) + 1 for grade in range(2, number_of + 1)]
    rest, counts = total - bound - (number_of - 1), [1] * (number_of - 1)
    while rest > 0:
        movable = [i for i in range(number_of - 1) if counts[i] < bound]
        whole, left = sum([loads[i] for i in movable]), rest
        for i in movable:
            addition = min(bound - counts[i], max(1, left * loads[i] // whole), rest)
            counts[i] = counts[i] + addition
            rest = rest - addition
    return np.array([bound] + counts)


def ragged(own_key, number_of, total, limit, skew):
    if number_of == 2:
        one = jax.random.randint(own_key, (), max(1, total - limit), min(limit, total - 1) + 1)
        return jnp.stack([one, total - one])
    sizes = jnp.asarray(split_up(number_of, total, limit, skew), jnp.int32)
    couples = (number_of - 1) // 2
    donor, receiver = sizes[1:1 + 2 * couples:2], sizes[2:2 + 2 * couples:2]
    slack = jnp.minimum(donor - 1, limit - receiver)
    moved = jax.random.randint(jax.random.fold_in(own_key, 1), (couples,), 0, 1 << 20) % (slack + 1)
    sizes = sizes.at[1:1 + 2 * couples:2].set(donor - moved).at[2:2 + 2 * couples:2].set(receiver + moved)
    return sizes[jax.random.permutation(jax.random.fold_in(own_key, 2), number_of)]


def routed_block(rng, own, number, rows, amount, top, reach, skew):
    ranking = jax.random.permutation(rng, amount)
    heavy_load, usual = load_shares(amount, rows * top, reach, skew, True), load_shares(amount, rows * top, reach, skew, False)
    places = jnp.arange(amount)

    def named(sizes, rotation):
        used = int((sizes > 0).sum())
        fixed = max(1, used // 4)
        passed = fixed + (places - fixed + rotation * (used - fixed)) % max(1, amount - fixed)
        return jnp.zeros((amount,), jnp.int32).at[ranking[jnp.where(places < fixed, places, passed)]].set(jnp.asarray(sizes, jnp.int32))

    sizes = jnp.where(number % 4 == 0, named(heavy_load, number // 4), named(usual, number - number // 4 - 1))
    mixed = jax.random.permutation(jax.random.fold_in(own, 3), amount)
    donor, sink = mixed[0:amount // 2 * 2:2], mixed[1:amount // 2 * 2:2]
    margin = jnp.minimum(sizes[donor] - 1, reach - sizes[sink]) // 2
    margin = jnp.where((donor == ranking[0]) | (sink == ranking[0]) | (sizes[sink] == 0), 0, jnp.maximum(margin, 0))
    passed = jax.random.randint(jax.random.fold_in(own, 4), (amount // 2,), 0, 1 << 20) % (margin + 1)
    sizes = sizes.at[donor].add(-passed).at[sink].add(passed)
    labels = jnp.searchsorted(jnp.cumsum(sizes), jnp.arange(rows * top), side="right").astype(jnp.int32)
    table = labels.reshape(top, rows).T
    table = table[jax.random.permutation(jax.random.fold_in(own, 1), rows)]
    rotation = jax.random.randint(jax.random.fold_in(own, 2), (rows, 1), 0, top)
    return jnp.take_along_axis(table, (jnp.arange(top)[None, :] + rotation) % top, axis=1)


def load_shares(amount, total, reach, skew, full):
    portions = [(1 << 20) // math.isqrt(grade ** skew) + 1 for grade in range(1, amount + 1)]
    largest = reach if full else min(reach, max(-(-total // amount), total * portions[0] // sum(portions)))
    least = 1 if total - largest >= amount - 1 else 0
    given, rest = [largest] + [least] * (amount - 1), total - largest - least * (amount - 1)
    while rest > 0:
        free = [i for i in range(1, amount) if given[i] < largest] or [i for i in range(1, amount) if given[i] < reach]
        whole, budget = sum([portions[i] for i in free]), rest
        for i in free:
            more = min(reach - given[i], max(1, budget * portions[i] // whole), rest)
            given[i] = given[i] + more
            rest = rest - more
    return np.array(given)


def gaussian(key, shape, deviation, reach, pieces=(), held_as=jnp.bfloat16):
    drawn = jax.random.normal(key, shape, jnp.float32) * deviation
    if len(pieces) > 0:
        drawn = block_levels(key, shape, pieces, -0.22, 0.18) * drawn
    return jnp.clip(drawn, min=-reach, max=reach).astype(held_as)


def setup_inputs(seed: int = 0) -> dict:
    splits = jax.random.split(jax.random.key(seed), 22)
    tokens = gaussian(splits[0], (TOKENS, D), 1.0, 6.0, ((0, 32),))
    cache_keys = draw_cache_keys(jax.random.fold_in(splits[21], 71), 0)
    cache_values = gaussian(splits[2], (TOKENS, LEN, KVH * HDIM), 1.0, 6.0, ((0, 32),))
    cache_gates = draw_cache_gates(jax.random.fold_in(splits[21], 71), 0)
    lengths = ragged(splits[4], TOKENS, TOKENS * LEN // 2, LEN, 2).astype(jnp.int32)
    routes_keys = jax.random.split(jax.random.fold_in(splits[5], 1), TOKENS // SEQ_DEV)
    routes_turns = jax.random.permutation(jax.random.fold_in(splits[5], 3), TOKENS // SEQ_DEV)
    routes = jax.vmap(lambda own, number: routed_block(jax.random.fold_in(splits[5], 2), own, number, SEQ_DEV, EXPERTS, TOPK, 1, 2))(routes_keys, routes_turns).reshape((TOKENS, TOPK))
    route_logits = gaussian(splits[6], (TOKENS, TOPK), 1.0, 6.0, ((0, 32),), jnp.float32)
    attn_gain = jnp.clip(1.0 + 0.18 * jax.random.normal(splits[7], (D,), jnp.float32), 0.1, 1.9)
    w_query = gaussian(splits[8], (D, HEADS * HDIM), D ** -0.5, 0.125, ((1, 4),))
    w_keyval = gaussian(splits[9], (D, 2 * KVH * HDIM), D ** -0.5, 0.125, ((1, 4),))
    w_forget = gaussian(splits[10], (D, KVH), D ** -0.5, 0.125)
    forget_bias = jnp.clip(jax.random.uniform(splits[11], (KVH,), jnp.float32, -1.0, 3.0), -1.0, 3.0)
    w_out = gaussian(splits[12], (HEADS * HDIM, D), (HEADS * HDIM) ** -0.5, 0.125, ((1, 4),))
    mix_gain = jnp.clip(1.0 + 0.18 * jax.random.normal(splits[13], (D,), jnp.float32), 0.1, 1.9)
    ffn_gain = jnp.clip(1.0 + 0.18 * jax.random.normal(splits[14], (D,), jnp.float32), 0.1, 1.9)
    w_gate = gaussian(splits[15], (EXPERTS, D, FF), D ** -0.5, 0.125, ((0, 8), (2, 4)))
    w_lin = gaussian(splits[16], (EXPERTS, D, FF), D ** -0.5, 0.125, ((0, 8), (2, 4)))
    gate_bias = gaussian(splits[17], (EXPERTS, FF), 3.0, 12.0, ((0, 8), (1, 4)), jnp.float32)
    lin_bias = gaussian(splits[18], (EXPERTS, FF), 3.0, 12.0, ((0, 8), (1, 4)), jnp.float32)
    w_down = gaussian(splits[19], (EXPERTS, FF, D), FF ** -0.5, 0.125, ((0, 8), (1, 4)))
    post_gain = jnp.clip(1.0 + 0.18 * jax.random.normal(splits[20], (D,), jnp.float32), 0.1, 1.9)
    return dict(tokens=tokens, cache_keys=cache_keys, cache_values=cache_values, cache_gates=cache_gates, lengths=lengths, routes=routes, route_logits=route_logits, attn_gain=attn_gain, w_query=w_query, w_keyval=w_keyval, w_forget=w_forget, forget_bias=forget_bias, w_out=w_out, mix_gain=mix_gain, ffn_gain=ffn_gain, w_gate=w_gate, w_lin=w_lin, gate_bias=gate_bias, lin_bias=lin_bias, w_down=w_down, post_gain=post_gain)


NORM_EPS = 1e-06
SWIGLU_ALPHA = 1.702
SWIGLU_LIMIT = 7.0
NEG_LARGE = -1e+30

def to_half(values):
    return lax.optimization_barrier(values.astype(jnp.bfloat16)).astype(jnp.float32)

def rms_scale(values, gain):
    values = values.astype(jnp.float32)
    return values * lax.rsqrt(lax.optimization_barrier(jnp.mean(values * values, axis=-1, keepdims=True)) + NORM_EPS) * gain.astype(jnp.float32)

def clamped_unit(gate, linear):
    gate = jnp.minimum(gate, SWIGLU_LIMIT)
    linear = jnp.clip(linear, -SWIGLU_LIMIT, SWIGLU_LIMIT)
    return gate * jax.nn.sigmoid(SWIGLU_ALPHA * gate) * (linear + 1.0)

def attend_one(args):
    query, fresh, keys, values, gates, length, forget = args
    group = HEADS // KVH
    q_four = query.reshape(KVH, group, HDIM).astype(jnp.float32)
    k_four = keys.reshape(LEN, KVH, HDIM).astype(jnp.float32)
    v_four = values.reshape(LEN, KVH, HDIM).astype(jnp.float32)
    new_key = fresh[:KVH * HDIM].reshape(KVH, HDIM).astype(jnp.float32)
    new_value = fresh[KVH * HDIM:].reshape(KVH, HDIM).astype(jnp.float32)
    place = jnp.arange(LEN, dtype=jnp.int32)
    last = lax.optimization_barrier(jnp.sum(jnp.where(place[None, :] == length - 1, gates, 0.0), axis=1))
    base = last + forget
    scale = HDIM ** (-0.5)
    scores = jnp.einsum('gqd,pgd->gqp', q_four, k_four) * scale + (base[:, None, None] - gates[:, None, :])
    live = place[None, None, :] < length
    masked = jnp.where(live, scores, NEG_LARGE)
    own = jnp.einsum('gqd,gd->gq', q_four, new_key) * scale
    top = jnp.maximum(lax.optimization_barrier(jnp.max(masked, axis=-1)), own)
    expo = jnp.where(live, jnp.exp(masked - top[..., None]), 0.0)
    own_expo = jnp.exp(own - top)
    total = lax.optimization_barrier(jnp.sum(expo, axis=-1)) + own_expo
    weights = to_half(expo / total[..., None])
    own_weight = to_half(own_expo / total)
    mixed = jnp.einsum('gqp,pgd->gqd', weights, v_four) + own_weight[..., None] * new_value[:, None, :]
    return mixed.reshape(HEADS * HDIM).astype(jnp.bfloat16)

def reference(tokens, cache_keys, cache_values, cache_gates, lengths, routes, route_logits, attn_gain, w_query, w_keyval, w_forget, forget_bias, w_out, mix_gain, ffn_gain, w_gate, w_lin, gate_bias, lin_bias, w_down, post_gain):
    normed = rms_scale(tokens, attn_gain).astype(jnp.bfloat16)
    query = jnp.dot(normed, w_query, preferred_element_type=jnp.float32).astype(jnp.bfloat16)
    fresh = jnp.dot(normed, w_keyval, preferred_element_type=jnp.float32).astype(jnp.bfloat16)
    forget = jax.nn.log_sigmoid(jnp.dot(normed, w_forget, preferred_element_type=jnp.float32) + forget_bias.astype(jnp.float32))
    mixed = lax.map(attend_one, (query, fresh, cache_keys, cache_values, cache_gates, lengths.astype(jnp.int32), forget))
    projected = jnp.dot(mixed, w_out, preferred_element_type=jnp.float32).astype(jnp.bfloat16)
    residual = tokens.astype(jnp.float32) + rms_scale(projected, mix_gain)
    expert_in = rms_scale(residual, ffn_gain).astype(jnp.bfloat16)
    hit = (routes[:, :, None] == jnp.arange(EXPERTS, dtype=jnp.int32)[None, None, :]).astype(jnp.float32)
    probs = jax.nn.softmax(route_logits.astype(jnp.float32), axis=-1)
    combine = lax.optimization_barrier(jnp.sum(probs[:, :, None] * hit, axis=1))

    def expert_step(total, items):
        gate_w, lin_w, gate_b, lin_b, down_w, share = items
        gate = jnp.dot(expert_in, gate_w, preferred_element_type=jnp.float32) + gate_b.astype(jnp.float32)
        linear = jnp.dot(expert_in, lin_w, preferred_element_type=jnp.float32) + lin_b.astype(jnp.float32)
        act = clamped_unit(gate, linear).astype(jnp.bfloat16)
        blocked = act.reshape(TOKENS, N_TP, FF // N_TP).astype(jnp.float32)
        down_blocks = down_w.reshape(N_TP, FF // N_TP, D).astype(jnp.float32)
        parts = to_half(jnp.einsum('tnf,nfd->ntd', blocked, down_blocks))
        expert_out = to_half(lax.optimization_barrier(jnp.sum(parts, axis=0)))
        return (total + share[:, None] * expert_out, None)
    moe, _ = lax.scan(expert_step, jnp.zeros((TOKENS, D), jnp.float32), (w_gate, w_lin, gate_bias, lin_bias, w_down, combine.T))
    updated = (residual + rms_scale(moe, post_gain)).astype(jnp.bfloat16)
    return (updated, fresh)
```

```python
import functools

import jax
import jax.numpy as jnp
from jax import lax
from jax.experimental import pallas as pl
from jax.experimental.pallas import tpu as pltpu
from jax.sharding import PartitionSpec as P

HEADS = 16
KVH = 2
HDIM = 128


NORM_EPS = 1e-06
SWIGLU_ALPHA = 1.702
SWIGLU_LIMIT = 7.0
NEG_LARGE = -1e30


def rms_scale(values, gain):
    values = values.astype(jnp.float32)
    return values * lax.rsqrt(jnp.mean(values * values, axis=-1, keepdims=True) + NORM_EPS) * gain


def clamped_unit(gate, linear):
    gate = jnp.minimum(gate, SWIGLU_LIMIT)
    linear = jnp.clip(linear, -SWIGLU_LIMIT, SWIGLU_LIMIT)
    return gate * jax.nn.sigmoid(SWIGLU_ALPHA * gate) * (linear + 1.0)


def block_scores(q_four, cache_keys, cache_gates, base, lengths, span, scale):
    seqs = cache_keys.shape[0]
    k_four = cache_keys.reshape(seqs, span, q_four.shape[1], q_four.shape[3])
    scores = (
        jnp.einsum("sgqd,spgd->sgqp", q_four, k_four, preferred_element_type=jnp.float32) * scale
    )
    scores = scores + (base[:, :, None, None] - cache_gates[:, :, None, :])
    place = lax.iota(jnp.int32, span)
    live = place[None, None, None, :] < lengths[:, None, None, None]
    return (jnp.where(live, scores, NEG_LARGE), live)


def per_device(
    tokens,
    cache_keys,
    cache_values,
    cache_gates,
    lengths,
    routes,
    route_logits,
    attn_gain,
    w_query,
    w_keyval,
    w_forget,
    forget_bias,
    w_out,
    mix_gain,
    ffn_gain,
    w_gate,
    w_lin,
    gate_bias,
    lin_bias,
    w_down,
    post_gain,
):
    seqs, width = tokens.shape
    normed = rms_scale(tokens, attn_gain).astype(jnp.bfloat16)
    query_cols = w_query.shape[1]
    pair_cols = w_keyval.shape[1]
    piece = lax.all_gather(normed, "tp", axis=0, tiled=True)
    both = jnp.concatenate(
        [
            jnp.dot(piece, w_query, preferred_element_type=jnp.float32),
            jnp.dot(piece, w_keyval, preferred_element_type=jnp.float32),
        ],
        axis=1,
    )
    gathered = both.astype(jnp.bfloat16)
    owned = lax.all_to_all(gathered, "tp", split_axis=0, concat_axis=1, tiled=True)
    groups = lax.axis_size("tp")
    owned = owned.reshape(seqs, groups, query_cols + pair_cols)
    query = owned[:, :, :query_cols].reshape(seqs, groups * query_cols)
    fresh = owned[:, :, query_cols:].reshape(seqs, groups * pair_cols)
    forget = jax.nn.log_sigmoid(
        jnp.dot(normed, w_forget, preferred_element_type=jnp.float32) + forget_bias
    )
    q_four = query.reshape(seqs, KVH, HEADS // KVH, HDIM)
    new_key = fresh[:, : KVH * HDIM].reshape(seqs, KVH, HDIM)
    new_value = fresh[:, KVH * HDIM :].reshape(seqs, KVH, HDIM)
    span_all = cache_keys.shape[1]
    place = lax.iota(jnp.int32, span_all)
    last = jnp.sum(
        jnp.where(place[None, None, :] == lengths[:, None, None] - 1, cache_gates, 0.0), axis=2
    )
    base = last + forget
    scale = HDIM ** (-0.5)
    own = jnp.einsum("sgqd,sgd->sgq", q_four, new_key, preferred_element_type=jnp.float32) * scale
    values_four = cache_values.reshape(seqs, span_all, KVH, HDIM)
    masked, live = block_scores(q_four, cache_keys, cache_gates, base, lengths, span_all, scale)
    top = jnp.maximum(jnp.max(masked, axis=-1), own)
    expo = jnp.where(live, jnp.exp(masked - top[..., None]), 0.0)
    own_expo = jnp.exp(own - top)
    total = jnp.sum(expo, axis=-1) + own_expo
    weights = (expo / total[..., None]).astype(jnp.bfloat16)
    mixed = jnp.einsum("sgqp,spgd->sgqd", weights, values_four, preferred_element_type=jnp.float32)
    own_weight = (own_expo / total).astype(jnp.bfloat16)
    mixed = (
        mixed
        + own_weight.astype(jnp.float32)[..., None] * new_value.astype(jnp.float32)[:, :, None, :]
    )
    mixed = mixed.reshape(seqs, HEADS * HDIM).astype(jnp.bfloat16)
    projected = jnp.dot(
        lax.all_gather(mixed, "tp", axis=0, tiled=True), w_out, preferred_element_type=jnp.float32
    ).astype(jnp.bfloat16)
    projected = lax.all_to_all(projected, "tp", split_axis=0, concat_axis=1, tiled=True)
    residual = tokens.astype(jnp.float32) + rms_scale(projected, mix_gain)
    expert_in = rms_scale(residual, ffn_gain).astype(jnp.bfloat16)
    experts = lax.axis_size("ep")
    hit = (routes[:, :, None] == lax.iota(jnp.int32, experts)[None, None, :]).astype(jnp.float32)
    probs = jax.nn.softmax(route_logits, axis=-1)
    combine = jnp.sum(probs[:, :, None] * hit, axis=1)
    chosen = jnp.sum(hit, axis=1).T
    outbound = jnp.where(
        chosen[:, :, None] > 0.5, expert_in[None, :, :], jnp.zeros((), jnp.bfloat16)
    )
    slots = outbound.shape[1]
    arrived = lax.all_to_all(outbound, "ep", split_axis=0, concat_axis=0, tiled=True)
    flat = arrived.reshape(experts * slots, width)
    pooled = lax.all_gather(flat, "tp", axis=0, tiled=True)
    piece = pooled
    gate = jnp.dot(piece, w_gate[0], preferred_element_type=jnp.float32) + gate_bias[0]
    linear = jnp.dot(piece, w_lin[0], preferred_element_type=jnp.float32) + lin_bias[0]
    act = clamped_unit(gate, linear).astype(jnp.bfloat16)
    summed = lax.psum_scatter(
        jnp.dot(act, w_down[0], preferred_element_type=jnp.float32).astype(jnp.bfloat16),
        "tp",
        scatter_dimension=0,
        tiled=True,
    )
    returned = lax.all_to_all(
        summed.reshape(experts, slots, width), "ep", split_axis=0, concat_axis=0, tiled=True
    )
    moe = jnp.einsum("se,esd->sd", combine, returned.astype(jnp.float32))
    updated = (residual + rms_scale(moe, post_gain)).astype(jnp.bfloat16)
    return (updated, fresh)


MESH = pl.DeviceIdType.MESH
F32 = jnp.float32
BF16 = jnp.bfloat16


def flip(value, mask, size):
    out, bit = value, 1
    while bit < size:
        if mask & bit:
            out = out + bit - 2 * bit * lax.rem(value // bit, 2)
        bit *= 2
    return out


def wait_bytes(ref, sem):
    pltpu.make_async_copy(ref, ref, sem).wait()


def block_rms(block, width):
    squares = jnp.sum(block * block, axis=1, keepdims=True)
    return lax.rsqrt(jnp.sum(squares, axis=0, keepdims=True) * (1.0 / width) + NORM_EPS)


def fused_kernel(
    n_ep,
    n_tp,
    tokens,
    cache_keys,
    cache_values,
    cache_gates,
    lengths,
    routes,
    route_logits,
    attn_gain,
    w_query,
    w_keyval,
    w_forget,
    forget_bias,
    w_out,
    mix_gain,
    mix_gain_l,
    ffn_gain,
    w_gate,
    w_lin,
    gate_bias,
    lin_bias,
    w_down,
    post_gain_l,
    updated,
    fresh,
    v_kv,
    v_gates,
    v_lengths,
    v_logits,
    v_again,
    v_qkv,
    v_forget,
    v_fbias,
    v_out,
    v_mgain,
    v_mgain_l,
    v_fgain,
    v_gl,
    v_gbias,
    v_lbias,
    v_down,
    v_pgain_l,
    tok_all,
    rt_all,
    qkv_out,
    qkv_all,
    mix_all,
    proj_out,
    proj_all,
    tok_out,
    tok_far,
    disp_out,
    disp_all,
    part_out,
    part_all,
    s_tok,
    s_qkv,
    s_mix,
    s_proj,
    s_far,
    s_disp,
    s_part,
    s_tok_l,
    s_proj_l,
    s_share,
    load_sem,
    tok_sem,
    rt_sem,
    qkv_sem,
    mix_sem,
    proj_sem,
    far_sem,
    disp_sem,
    part_sem,
    near_sem,
):
    my_ep, my_tp = lax.axis_index("ep"), lax.axis_index("tp")
    seqs, width = tokens.shape
    group = n_tp * seqs
    slots = n_ep * n_tp
    qc = w_query.shape[1]
    oc = w_out.shape[1]
    ff = w_down.shape[1]
    blocks = width // 128
    q_sub = qc // HDIM
    heads = HEADS
    per = HEADS // KVH
    scale = HDIM ** (-0.5)

    ep_at = [flip(my_ep, k, n_ep) for k in range(n_ep)]
    tp_at = [flip(my_tp, k, n_tp) for k in range(n_tp)]
    me = my_ep * n_tp + my_tp

    def tell(sem, ep, tp):
        pl.semaphore_signal(sem, inc=1, device_id=(ep, tp), device_id_type=MESH)

    def tell_near(sem):
        tell(sem, ep_at[1], my_tp)

        @pl.when(my_ep >= 2)
        def _():
            tell(sem, my_ep - 2, my_tp)

        @pl.when(my_ep + 2 < n_ep)
        def _():
            tell(sem, my_ep + 2, my_tp)

    near = 1 + jnp.minimum(my_ep // 2, 1) + jnp.minimum((n_ep - 1 - my_ep) // 2, 1)

    def heard(k):
        pl.semaphore_wait(near_sem.at[k], near)

    load_list, waits = [], {}

    def load(key, *pairs, whole=None):
        k = len(waits)
        load_list.extend((a, b, k) for a, b in pairs)
        waits[key] = (pairs[0][1] if whole is None else whole, k)

    def loaded(*keys):
        for key in keys:
            ref, k = waits[key]
            wait_bytes(ref, load_sem.at[k])

    load("tok", (tokens, tok_all.at[0]))
    load("rt", (routes, rt_all.at[0]))
    load("again", (attn_gain, v_again))
    load("qkv", (w_query, v_qkv.at[:, :qc]), (w_keyval, v_qkv.at[:, qc:]), whole=v_qkv)
    load("forget", (w_forget, v_forget))
    load("fbias", (forget_bias, v_fbias))
    load("lengths", (lengths, v_lengths))
    load("gates", (cache_gates, v_gates))
    load("kv", (cache_keys, v_kv.at[0]), (cache_values, v_kv.at[1]), whole=v_kv)
    load("out", (w_out, v_out))
    load("mgain", (mix_gain, v_mgain))
    load("mgain_l", (mix_gain_l, v_mgain_l))
    load("fgain", (ffn_gain, v_fgain))
    load("gl", (w_gate.at[0], v_gl.at[:, :ff]), (w_lin.at[0], v_gl.at[:, ff:]), whole=v_gl)
    load("gbias", (gate_bias, v_gbias))
    load("lbias", (lin_bias, v_lbias))
    load("down", (w_down.at[0], v_down))
    load("logits", (route_logits, v_logits))
    load("pgain_l", (post_gain_l, v_pgain_l))

    barrier = pltpu.get_barrier_semaphore()
    for j in range(n_tp - 1, 0, -1):
        tell(barrier, my_ep, tp_at[j])
    copies = [pltpu.make_async_copy(a, b, load_sem.at[k]) for a, b, k in load_list]
    copies[0].start()
    tell_near(barrier)
    for copy in copies[1:]:
        copy.start()

    def tp_send(src, dst, sem):
        for j in range(n_tp - 1, 0, -1):
            pltpu.make_async_remote_copy(
                src_ref=src(tp_at[j]),
                dst_ref=dst.at[j],
                send_sem=sem.at[0],
                recv_sem=sem.at[1],
                device_id=(my_ep, tp_at[j]),
                device_id_type=MESH,
            ).start()

    sent = []

    def arrive(ref, sem):
        wait_bytes(ref.at[pl.ds(1, ref.shape[0] - 1)], sem.at[1])
        sent.append((ref, sem))

    loaded("tok", "rt")
    pl.semaphore_wait(barrier, n_tp - 1 + near)
    tp_send(lambda p: tok_all.at[0], tok_all, tok_sem)
    tp_send(lambda p: rt_all.at[0], rt_all, rt_sem)
    tell_near(near_sem.at[0])
    s_qkv[...] = jnp.zeros_like(s_qkv)
    loaded("again", "qkv")
    arrive(tok_all, tok_sem)

    for s in range(n_tp):
        piece = tok_all[tp_at[s]].astype(F32)
        for b in range(blocks):
            s_tok[b, s * seqs : (s + 1) * seqs, :] = piece[:, b * 128 : (b + 1) * 128]
    toks = jnp.concatenate([s_tok[b] for b in range(blocks)], axis=1)
    normed = rms_scale(toks, v_again[...]).astype(BF16)
    both = jnp.dot(normed, v_qkv[...], preferred_element_type=F32)
    for c in range(q_sub + 1):
        s_qkv[pl.ds(c, group, stride=8), :] = both[:, c * HDIM : (c + 1) * HDIM]
    for s in range(n_tp):
        qkv_out[s] = s_qkv[s * seqs * 8 : (s + 1) * seqs * 8, :].astype(BF16)
    tp_send(lambda p: qkv_out.at[p], qkv_all, qkv_sem)
    heard(0)
    tell_near(near_sem.at[1])
    qkv_all[0] = qkv_out[my_tp]

    loaded("forget", "fbias", "lengths", "gates")
    own_normed = rms_scale(tok_all[0], v_again[...]).astype(BF16)
    raw = lax.dot_general(
        own_normed, v_forget[...], (((1,), (1,)), ((), ())), preferred_element_type=F32
    )
    raw = raw + v_fbias[...]
    forget = jnp.minimum(raw, 0.0) - jnp.log1p(jnp.exp(-jnp.abs(raw)))
    span = cache_keys.shape[1]
    place = lax.broadcasted_iota(jnp.int32, (1, span), 1)
    first = lax.broadcasted_iota(jnp.int32, (heads, 1), 0) < per
    shifts, lives = [], []
    for t in range(seqs):
        length = v_lengths[0:1, t : t + 1]
        gates = v_gates[t]
        last = jnp.sum(jnp.where(place == length - 1, gates, 0.0), axis=1, keepdims=True)
        rows = []
        for g in range(KVH):
            base = last[g : g + 1] + forget[t : t + 1, g : g + 1]
            rows.append(base - gates[g : g + 1])
        shifts.append(jnp.where(first, rows[0], rows[1]))
        lives.append(place < length)
    heard(1)
    tell_near(near_sem.at[2])
    loaded("kv")
    arrive(qkv_all, qkv_sem)

    pieces = [qkv_all[tp_at[s]].astype(F32) for s in range(n_tp)]
    entries = []
    for t in range(seqs):
        q = jnp.concatenate([p[t * 8 : t * 8 + q_sub] for p in pieces], axis=0)
        e = [p[t * 8 + q_sub : t * 8 + q_sub + 1] for p in pieces]
        entries.append(jnp.concatenate(e, axis=1))
        own = jnp.sum(q * jnp.where(first, e[0], e[1]), axis=1, keepdims=True) * scale
        q_wide = jnp.concatenate(
            [jnp.where(first, q, 0.0), jnp.where(first, 0.0, q)], axis=1
        ).astype(BF16)
        scores = lax.dot_general(
            q_wide, v_kv[0, t], (((1,), (1,)), ((), ())), preferred_element_type=F32
        )
        masked = jnp.where(lives[t], scores * scale + shifts[t], NEG_LARGE)
        top = jnp.maximum(jnp.max(masked, axis=1, keepdims=True), own)
        expo = jnp.exp(masked - top)
        own_expo = jnp.exp(own - top)
        total = jnp.sum(expo, axis=1, keepdims=True) + own_expo
        wide = jnp.dot(expo.astype(BF16), v_kv[1, t], preferred_element_type=F32)
        mixed = jnp.where(first, wide[:, :HDIM], wide[:, HDIM:])
        mixed = (mixed + own_expo * jnp.where(first, e[2], e[3])) / total
        mix_all[0, t * heads : (t + 1) * heads, :] = mixed.astype(BF16)
    tp_send(lambda p: mix_all.at[0], mix_all, mix_sem)
    fresh[...] = jnp.concatenate(entries, axis=0).astype(BF16)

    arrive(rt_all, rt_sem)
    named = []
    for c in range(seqs):
        rows = jnp.concatenate([rt_all[tp_at[s]][c : c + 1] for s in range(n_tp)], axis=0)
        picks = [
            jnp.broadcast_to(rows[:, k : k + 1], (n_tp, 128)) for k in range(routes.shape[1])
        ]
        named.append(picks)

    def chosen(c, e):
        hit = named[c][0] == e
        for k in range(1, routes.shape[1]):
            hit = jnp.logical_or(hit, named[c][k] == e)
        return hit

    masks = [[chosen(c, e) for e in range(n_ep)] for c in range(1, seqs)]

    def choose(scratch, columns, out):
        for b in range(columns // 128):
            lanes = slice(b * 128, (b + 1) * 128)
            rows = [scratch[b, pl.ds(c, n_tp, stride=seqs), :] for c in range(seqs)]
            for e in range(n_ep):
                row = rows[0]
                for c in range(1, seqs):
                    row = jnp.where(masks[c - 1][e], rows[c], row)
                out[e, :, lanes] = row.astype(BF16)

    choose(s_tok, width, tok_out)
    heard(2)
    tell_near(near_sem.at[3])
    for i in range(n_ep - 1, 0, -1):
        pltpu.make_async_remote_copy(
            src_ref=tok_out.at[ep_at[i]],
            dst_ref=tok_far.at[i],
            send_sem=far_sem.at[0],
            recv_sem=far_sem.at[1],
            device_id=(ep_at[i], my_tp),
            device_id_type=MESH,
        ).start()
    tok_far[0] = tok_out[my_ep]

    for b in range(blocks):
        s_tok_l[pl.ds(b, seqs, stride=blocks), :] = tok_all[0, :, b * 128 : (b + 1) * 128].astype(
            F32
        )
    loaded("out", "mgain", "mgain_l", "fgain", "gl", "gbias", "lbias", "down", "logits", "pgain_l")
    logits = v_logits[...]
    odds = jnp.exp(logits - jnp.max(logits, axis=1, keepdims=True))
    probs = odds / jnp.sum(odds, axis=1, keepdims=True)
    mine = rt_all[0]
    for t in range(seqs):
        at = [jnp.broadcast_to(mine[t : t + 1, c : c + 1], (8, 128)) for c in range(mine.shape[1])]
        of = [jnp.broadcast_to(probs[t : t + 1, c : c + 1], (8, 128)) for c in range(len(at))]
        for e in range(n_ep):
            share = jnp.where(at[0] == e, of[0], 0.0)
            for c in range(1, len(at)):
                share = share + jnp.where(at[c] == e, of[c], 0.0)
            s_share[t, e] = share
    heard(3)
    arrive(mix_all, mix_sem)

    for s in range(n_tp):
        size = seqs * heads
        s_mix[s * size : (s + 1) * size, :] = mix_all[tp_at[s]].astype(F32)
    mixed_all = jnp.concatenate(
        [s_mix[pl.ds(h, group, stride=heads), :] for h in range(heads)], axis=1
    ).astype(BF16)
    proj = jnp.dot(mixed_all, v_out[...], preferred_element_type=F32)
    for b in range(oc // 128):
        s_proj[b] = proj[:, b * 128 : (b + 1) * 128]
    choose(s_proj, oc, disp_out)

    def all_send(src, dst, sem):
        for i in range(n_ep - 1, -1, -1):
            for j in range(n_tp - 1, -1, -1):
                if i or j:
                    pltpu.make_async_remote_copy(
                        src_ref=src(ep_at[i], tp_at[j]),
                        dst_ref=dst.at[i * n_tp + j],
                        send_sem=sem.at[0],
                        recv_sem=sem.at[1],
                        device_id=(ep_at[i], tp_at[j]),
                        device_id_type=MESH,
                    ).start()

    all_send(lambda ep, tp: disp_out.at[ep], disp_all, disp_sem)
    disp_all[0] = disp_out[my_ep]
    for s in range(n_tp):
        proj_out[s] = proj[s * seqs : (s + 1) * seqs].astype(BF16)
    tp_send(lambda p: proj_out.at[p], proj_all, proj_sem)
    proj_all[0] = proj_out[my_tp]
    arrive(tok_far, far_sem)
    for e in range(n_ep):
        s_far[e * n_tp : (e + 1) * n_tp, :] = tok_far[ep_at[e]].astype(F32)

    arrive(disp_all, disp_sem)
    for e in range(n_ep):
        for r in range(n_tp):
            s_disp[e * n_tp : (e + 1) * n_tp, r * oc : (r + 1) * oc] = disp_all[
                ep_at[e] * n_tp + tp_at[r]
            ].astype(F32)
    arrived = s_far[...] + rms_scale(s_disp[...], v_mgain[...])
    power = lax.rsqrt(jnp.mean(arrived * arrived, axis=1, keepdims=True) + NORM_EPS)
    expert_in = (arrived * v_fgain[...]).astype(BF16)
    hidden = jnp.dot(expert_in, v_gl[...], preferred_element_type=F32) * power
    act = clamped_unit(hidden[:, :ff] + v_gbias[...], hidden[:, ff:] + v_lbias[...]).astype(BF16)
    parts = jnp.dot(act, v_down[...], preferred_element_type=F32)
    for b in range(blocks):
        s_part[pl.ds(b, slots, stride=blocks), :] = parts[:, b * 128 : (b + 1) * 128]
    for s in range(slots):
        part_out[s] = s_part[s * blocks : (s + 1) * blocks, :].astype(BF16)
    all_send(lambda ep, tp: part_out.at[ep * n_tp + tp], part_all, part_sem)
    part_all[0] = part_out[me]

    arrive(proj_all, proj_sem)
    for s in range(n_tp):
        piece = proj_all[tp_at[s]].astype(F32)
        for b in range(oc // 128):
            s_proj_l[pl.ds(s * (oc // 128) + b, seqs, stride=blocks), :] = piece[
                :, b * 128 : (b + 1) * 128
            ]
    residual = []
    for t in range(seqs):
        rows = slice(t * blocks, (t + 1) * blocks)
        own_proj = s_proj_l[rows, :]
        residual.append(s_tok_l[rows, :] + own_proj * block_rms(own_proj, width) * v_mgain_l[...])

    arrive(part_all, part_sem)
    moe = [jnp.zeros((blocks, 128), F32) for _ in range(seqs)]
    for e in range(n_ep):
        summed = part_all[ep_at[e] * n_tp + tp_at[0]].astype(F32)
        for r in range(1, n_tp):
            summed = summed + part_all[ep_at[e] * n_tp + tp_at[r]].astype(F32)
        summed = summed.astype(BF16).astype(F32)
        for t in range(seqs):
            share = jnp.concatenate([s_share[t, e]] * (blocks // 8), axis=0)
            moe[t] = moe[t] + summed * share
    for t in range(seqs):
        rows = slice(t * blocks, (t + 1) * blocks)
        updated[rows, :] = residual[t] + moe[t] * block_rms(moe[t], width) * v_pgain_l[...]
    for ref, sem in sent:
        wait_bytes(ref.at[pl.ds(1, ref.shape[0] - 1)], sem.at[0])


def fused_device(n_ep, n_tp, *args):
    args = [a.reshape(1, -1) if a.ndim == 1 else a for a in args]
    (tokens, keys, values, gates, lengths, routes, logits, again, wq, wkv, wf, fb, wo, mg, fg,
     wg, wl, gb, lb, wd, pg) = args
    seqs, width = tokens.shape
    blocks = width // 128
    mg_l, pg_l, wf = mg.reshape(blocks, 128), pg.reshape(blocks, 128), wf.T
    both = wq.shape[1] + wkv.shape[1]
    ff, oc = wd.shape[1], wo.shape[1]
    slots, group = n_ep * n_tp, n_tp * seqs
    vmem = pltpu.VMEM
    dma = pltpu.SemaphoreType.DMA

    def like(a):
        return vmem(a.shape, a.dtype)

    operands = [tokens, keys, values, gates, lengths, routes, logits, again, wq, wkv, wf, fb, wo,
                mg, mg_l, fg, wg, wl, gb, lb, wd, pg_l]
    scratch = [
        vmem((2,) + keys.shape, keys.dtype),
        like(gates),
        like(lengths),
        like(logits),
        like(again),
        vmem((width, both), wq.dtype),
        like(wf),
        like(fb),
        like(wo),
        like(mg),
        like(mg_l),
        like(fg),
        vmem((width, 2 * ff), wg.dtype),
        like(gb),
        like(lb),
        vmem(wd.shape[1:], wd.dtype),
        like(pg_l),
        vmem((n_tp, seqs, width), tokens.dtype),
        vmem((n_tp,) + routes.shape, routes.dtype),
        vmem((n_tp, seqs * 8, HDIM), BF16),
        vmem((n_tp, seqs * 8, HDIM), BF16),
        vmem((n_tp, seqs * HEADS, HDIM), BF16),
        vmem((n_tp, seqs, oc), BF16),
        vmem((n_tp, seqs, oc), BF16),
        vmem((n_ep, n_tp, width), BF16),
        vmem((n_ep, n_tp, width), BF16),
        vmem((n_ep, n_tp, oc), BF16),
        vmem((slots, n_tp, oc), BF16),
        vmem((slots, blocks, 128), BF16),
        vmem((slots, blocks, 128), BF16),
        vmem((blocks, group, 128), F32),
        vmem((group * 8, HDIM), F32),
        vmem((group * HEADS, HDIM), F32),
        vmem((oc // 128, group, 128), F32),
        vmem((slots, width), F32),
        vmem((slots, width), F32),
        vmem((slots * blocks, 128), F32),
        vmem((seqs * blocks, 128), F32),
        vmem((seqs * blocks, 128), F32),
        vmem((seqs, n_ep, 8, 128), F32),
        dma((19,)),
        dma((2,)),
        dma((2,)),
        dma((2,)),
        dma((2,)),
        dma((2,)),
        dma((2,)),
        dma((2,)),
        dma((2,)),
        pltpu.SemaphoreType.REGULAR((4,)),
    ]
    return pl.pallas_call(
        functools.partial(fused_kernel, n_ep, n_tp),
        out_shape=(
            vmem((seqs * blocks, 128), F32),
            vmem((seqs, n_tp * wkv.shape[1]), BF16),
        ),
        in_specs=[pl.BlockSpec(memory_space=pl.ANY)] * len(operands),
        out_specs=(pl.BlockSpec(memory_space=vmem), pl.BlockSpec(memory_space=vmem)),
        scratch_shapes=scratch,
        compiler_params=pltpu.CompilerParams(
            collective_id=0, has_side_effects=True, vmem_limit_bytes=66_000_000
        ),
        name="decode_layer",
    )(*operands)


def hand_over(updated, fresh, updated_out, fresh_out):
    seqs, width = updated_out.shape
    for b in range(width // 128):
        updated_out[:, b * 128 : (b + 1) * 128] = updated[
            pl.ds(b, seqs, stride=width // 128), :
        ].astype(BF16)
    fresh_out[...] = fresh[...]


def plain_copy(results, seqs):
    vmem = pl.BlockSpec(memory_space=pltpu.VMEM)
    updated, fresh = [pltpu.with_memory_space_constraint(r, pltpu.VMEM) for r in results]
    return pl.pallas_call(
        hand_over,
        out_shape=(
            jax.ShapeDtypeStruct((seqs, updated.size // seqs), BF16),
            jax.ShapeDtypeStruct(fresh.shape, BF16),
        ),
        in_specs=[vmem, vmem],
        out_specs=(vmem, vmem),
        name="hand_over",
    )(updated, fresh)


def fits(args, n_ep, n_tp):
    tokens, keys, wq, wkv, wo = args[0], args[1], args[8], args[9], args[12]
    seqs, width = tokens.shape
    return (
        n_ep in (2, 4, 8)
        and n_tp == 2 * KVH
        and n_tp * seqs == 8
        and seqs > 1
        and KVH == 2
        and wq.shape[1] % HDIM == 0
        and wq.shape[1] // HDIM < 8
        and wkv.shape[1] == HDIM
        and HDIM == 128
        and HEADS % 16 == 0
        and wo.shape[1] % 128 == 0
        and width % 2048 == 0
    )


def solution(mesh):
    in_specs = (
        P(("ep", "tp"), None),
        P(("ep", "tp"), None, None),
        P(("ep", "tp"), None, None),
        P(("ep", "tp"), None, None),
        P(("ep", "tp")),
        P(("ep", "tp"), None),
        P(("ep", "tp"), None),
        P(),
        P(None, "tp"),
        P(None, "tp"),
        P(),
        P(),
        P(None, "tp"),
        P(),
        P(),
        P("ep", None, "tp"),
        P("ep", None, "tp"),
        P("ep", "tp"),
        P("ep", "tp"),
        P("ep", "tp", None),
        P(),
    )
    out_specs = (P(("ep", "tp"), None), P(("ep", "tp"), None))
    n_ep, n_tp = mesh.shape["ep"], mesh.shape["tp"]

    def body(*args):
        if fits(args, n_ep, n_tp):
            return plain_copy(fused_device(n_ep, n_tp, *args), args[0].shape[0])
        return per_device(*args)

    return jax.shard_map(
        body, mesh=mesh, in_specs=in_specs, out_specs=out_specs, check_vma=False
    )
```
